32 devices in a mesh: dp: 4 (over y, x), kv: 4 (over z), tp: 2 (over core).
Axes of the slice: x: 2, y: 2, z: 4, core: 2. Of those that a mesh axis runs over, the one named last changes fastest.
Arguments:
- tokens: bfloat16 [8192, 2048], P(('dp', 'kv')), parts along dimension 0, may hold values from -60 to 60, as said below
- chosen: int32 [128, 16], P(('dp', 'kv')), parts along dimension 0, may hold values from -1 to 31, as said below
- query_weight: bfloat16 [2048, 1024], P('kv', 'tp'), may hold values from -0.125 to 0.125
- key_matrix: bfloat16 [2048, 128], P('kv', 'tp'), may hold values from -0.125 to 0.125
- value_matrix: bfloat16 [2048, 128], P('kv', 'tp'), may hold values from -0.125 to 0.125
- out_weight: bfloat16 [1024, 2048], P('tp', 'kv'), may hold values from -0.1875 to 0.1875
- out_gain: float32 [2048], replicated, may hold values from 0.1 to 1.9
Outputs:
- mixed_out: bfloat16 [8192, 2048], P(('dp', 'kv', 'tp')), parts along dimension 0
The draws below stay inside these ranges and needn't reach their ends.
There are 4 independent parts, one for each index of `dp`. The reference program is written for one: setup_inputs(seed, part) draws one part's arguments, and reference() takes and returns one part's arrays. A program takes and returns all parts, laid end to end along the dimension named above; an argument that names none is the same for every part. Nothing has to cross between parts.
Inputs may be any that keep to these rules, and one draw needn't show every extreme that they name: tokens are of order one apart from few rows. chosen[g, 0] = g; every other entry of row g is -1 or a block below g, and the entries of a row other than -1 are distinct; the blocks that the rows of one device name on any single other device are at most 2 different ones, and this is reached.
All inputs are finite; a program needn't handle non-finite values.
Results may differ from the reference program's by a relative error of at most 0.012.
The reference program's roundings to bfloat16 on the way count: a program that leaves them out, or rounds other values in their place, can miss the bound.
Values may be sent and summed in bfloat16 or wider, within the bound.
A program may use at most 64 MiB of HBM per device.

```python
import jax
import jax.numpy as jnp
from jax import lax

MODEL_WIDTH = 2048
QUERY_HEADS = 16
KEY_VALUE_HEADS = 2
HEAD_WIDTH = 64
BLOCK_LENGTH = 64
SEL = 16
CAP = 2
SEQ = 2048
BLOCKS_DEV = 8
SEQUENCE_BLOCKS = 32
N_KV = 4


def draw_tokens(key, part):
    base = jax.random.normal(key, (SEQ, MODEL_WIDTH), jnp.float32)
    return jnp.clip(base, -60.0, 60.0).astype(jnp.bfloat16)


def draw_chosen(key, part):
    owners = N_KV
    per_dev = BLOCKS_DEV
    parts_keys = jax.random.split(key, 3)
    requester = jnp.arange(owners, dtype=jnp.int32)[:, None]
    holder = jnp.arange(owners, dtype=jnp.int32)[None, :]
    roll = jax.random.randint(parts_keys[0], (owners, owners), 0, 8)
    favored = (holder == 0) | (holder == requester - 1) | (holder == requester - owners // 2)
    counts = jnp.where(favored | (roll < 2), CAP, jnp.where(roll < 4, 1, 0))
    counts = jnp.where(holder < requester, counts, 0)
    order = jax.random.randint(parts_keys[1], (owners, owners, per_dev), 0, 1 << 20) * 1024 + jnp.arange(per_dev, dtype=jnp.int32)
    _, first = lax.top_k(order, min(CAP, per_dev))
    first = jnp.concatenate([first, jnp.zeros((owners, owners, CAP - first.shape[-1]), jnp.int32)], axis=-1)
    slot_index = jnp.arange(CAP, dtype=jnp.int32)
    counts = jnp.minimum(counts, per_dev)
    remote_ids = (holder[:, :, None] * per_dev + first).reshape(owners, owners * CAP)
    remote_live = (slot_index[None, None, :] < counts[:, :, None]).reshape(owners, owners * CAP)
    remote_tier = jnp.broadcast_to(jnp.where(favored, 2, 1)[:, :, None], (owners, owners, CAP)).reshape(owners, owners * CAP)
    local_pos = jnp.arange(per_dev, dtype=jnp.int32)
    local_ids = jnp.broadcast_to((requester * per_dev + local_pos[None, :])[:, None, :], (owners, per_dev, per_dev))
    local_live = jnp.broadcast_to((local_pos[None, :] < local_pos[:, None])[None], (owners, per_dev, per_dev))
    pad_ids = jnp.zeros((owners, per_dev, SEL), jnp.int32)
    pad_live = jnp.zeros((owners, per_dev, SEL), bool)
    cand_ids = jnp.concatenate([jnp.broadcast_to(remote_ids[:, None, :], (owners, per_dev, owners * CAP)), local_ids, pad_ids], axis=-1)
    cand_live = jnp.concatenate([jnp.broadcast_to(remote_live[:, None, :], (owners, per_dev, owners * CAP)), local_live, pad_live], axis=-1)
    cand_tier = jnp.concatenate([jnp.broadcast_to(remote_tier[:, None, :], (owners, per_dev, owners * CAP)), jnp.ones((owners, per_dev, per_dev), jnp.int32), jnp.zeros((owners, per_dev, SEL), jnp.int32)], axis=-1)
    cand_width = owners * CAP + per_dev + SEL
    cand_index = jnp.arange(cand_width, dtype=jnp.int32)[None, None, :]
    noise = jax.random.randint(parts_keys[2], (owners, per_dev, cand_width), 0, 1 << 17)
    score = jnp.where(cand_live, cand_tier * (1 << 28) + noise * 2048 + cand_index, cand_index)
    _, position = lax.top_k(score, SEL - 1)
    taken = jnp.take_along_axis(cand_ids, position, axis=-1)
    live = jnp.take_along_axis(cand_live, position, axis=-1)
    others = jnp.where(live, taken, -1)
    own_ids = (requester * per_dev + local_pos[None, :])[:, :, None]
    return jnp.concatenate([own_ids, others], axis=-1).reshape(owners * per_dev, SEL).astype(jnp.int32)


def block_scale(key, dims, cuts, smallest, high):
    def one(dim, parts):
        heights = jax.random.uniform(jax.random.fold_in(jax.random.fold_in(key, 6), dim), (parts,), jnp.float32, smallest / len(cuts), high / len(cuts))
        return jnp.repeat(jnp.exp(heights), dims[dim] // parts).reshape((-1,) + (1,) * (len(dims) - dim - 1))

    gain = one(*cuts[0])
    for cut in cuts[1:]:
        gain = gain * one(*cut)
    return gain


def centred(stream_key, shape, spread, reach, shards=(), kind=jnp.bfloat16):
    gain = block_scale(stream_key, shape, shards, -0.22, 0.18) if shards else 1.0
    array = jax.random.normal(stream_key, shape, jnp.float32) * spread * gain
    return jnp.minimum(jnp.maximum(array, -reach), reach).astype(kind)


def setup_inputs(seed: int = 0, part: int = 0) -> dict:
    splits = jax.random.split(jax.random.key(seed), 8)
    own_keys = jax.random.split(jax.random.fold_in(splits[7], part), 8)
    return {
        "tokens": draw_tokens(jax.random.fold_in(jax.random.fold_in(splits[7], part), 71), part),
        "chosen": draw_chosen(jax.random.fold_in(jax.random.fold_in(splits[7], part), 71), part),
        "query_weight": centred(splits[2], (MODEL_WIDTH, QUERY_HEADS * HEAD_WIDTH), MODEL_WIDTH ** -0.5, 0.125, ((0, 4), (1, 2))),
        "key_matrix": centred(splits[3], (MODEL_WIDTH, KEY_VALUE_HEADS * HEAD_WIDTH), MODEL_WIDTH ** -0.5, 0.125, ((0, 4), (1, 2))),
        "value_matrix": centred(splits[4], (MODEL_WIDTH, KEY_VALUE_HEADS * HEAD_WIDTH), MODEL_WIDTH ** -0.5, 0.125, ((0, 4), (1, 2))),
        "out_weight": centred(splits[5], (QUERY_HEADS * HEAD_WIDTH, MODEL_WIDTH), (QUERY_HEADS * HEAD_WIDTH) ** -0.5, 0.1875, ((0, 2), (1, 4))),
        "out_gain": jnp.clip(1.0 + 0.18 * jax.random.normal(splits[6], (MODEL_WIDTH,), jnp.float32), 0.1, 1.9),
    }


def reference(tokens, chosen, query_weight, key_matrix, value_matrix, out_weight, out_gain):
    head_groups = QUERY_HEADS // KEY_VALUE_HEADS
    query_rows = jnp.dot(tokens, query_weight, preferred_element_type=jnp.float32).astype(jnp.bfloat16)
    key_rows = jnp.dot(tokens, key_matrix, preferred_element_type=jnp.float32).astype(jnp.bfloat16)
    value_rows = jnp.dot(tokens, value_matrix, preferred_element_type=jnp.float32).astype(jnp.bfloat16)
    blocked_queries = query_rows.reshape(SEQUENCE_BLOCKS, BLOCK_LENGTH, KEY_VALUE_HEADS, head_groups, HEAD_WIDTH)
    blocked_keys = key_rows.reshape(SEQUENCE_BLOCKS, BLOCK_LENGTH, KEY_VALUE_HEADS, HEAD_WIDTH)
    blocked_values = value_rows.reshape(SEQUENCE_BLOCKS, BLOCK_LENGTH, KEY_VALUE_HEADS, HEAD_WIDTH)
    offsets = jnp.arange(BLOCK_LENGTH, dtype=jnp.int32)
    score_scale = HEAD_WIDTH ** (-0.5)

    def one_block(inputs):
        block, row_ids, index = inputs
        safe_ids = jnp.maximum(row_ids, 0).astype(jnp.int32)
        picked_keys = blocked_keys[safe_ids].astype(jnp.float32)
        picked_values = blocked_values[safe_ids].astype(jnp.float32)
        query_pos = index * BLOCK_LENGTH + offsets
        key_pos = safe_ids[:, None] * BLOCK_LENGTH + offsets[None, :]
        visible = (row_ids >= 0)[None, :, None] & (key_pos[None, :, :] <= query_pos[:, None, None])
        scores = jnp.einsum('qhgd,skhd->hgqsk', block.astype(jnp.float32), picked_keys) * score_scale
        scores = jnp.where(visible[None, None], scores, -1e+30)
        row_max = lax.optimization_barrier(jnp.max(scores, axis=(3, 4), keepdims=True))
        expon = jnp.exp(scores - row_max)
        row_sum = lax.optimization_barrier(jnp.sum(expon, axis=(3, 4), keepdims=True))
        weights_bf = (expon / row_sum).astype(jnp.bfloat16)
        result = jnp.einsum('hgqsk,skhd->qhgd', weights_bf.astype(jnp.float32), picked_values)
        return result.astype(jnp.bfloat16)
    attended = lax.map(one_block, (blocked_queries, chosen, jnp.arange(SEQUENCE_BLOCKS, dtype=jnp.int32)))
    attended = attended.reshape(SEQ, QUERY_HEADS * HEAD_WIDTH)
    mixed = jnp.dot(attended, out_weight, preferred_element_type=jnp.float32)
    normed = mixed * lax.rsqrt(lax.optimization_barrier(jnp.mean(mixed * mixed, axis=-1, keepdims=True)) + 1e-06) * out_gain.astype(jnp.float32)
    return normed.astype(jnp.bfloat16)
```

```python
import functools

import jax
import jax.numpy as jnp
from jax import lax
from jax.experimental import pallas as pl
from jax.experimental.pallas import tpu as pltpu
from jax.sharding import PartitionSpec as P

HEAD_WIDTH = 64
BLOCK_LENGTH = 64
LANES = 2 * HEAD_WIDTH
HIDDEN = -1e30


def remote(src, dst, send, recv, axis, peer):
    return pltpu.make_async_remote_copy(
        src_ref=src,
        dst_ref=dst,
        send_sem=send,
        recv_sem=recv,
        device_id={axis: peer},
        device_id_type=pl.DeviceIdType.MESH,
    )


def fused(
    n_dp, n_kv, n_tp,
    chosen, tokens_hbm, pair_own, query_own, out_own, gain, result,
    tokens, pair_all, query_all, out_all, kv_all, vk_all, query_sum, query_rows, attended,
    leaving, arriving, kept,
    token_sem, z_send, z_recv, d_send, d_recv, kv_send, kv_recv, t_send, t_recv,
):
    d, z, t = lax.axis_index("dp"), lax.axis_index("kv"), lax.axis_index("tp")
    rows, width = tokens.shape
    blocks = rows // BLOCK_LENGTH
    depth = width // n_kv
    half = rows // n_tp
    token_copy = pltpu.make_async_copy(tokens_hbm, tokens, token_sem)
    token_copy.start()

    barrier = pltpu.get_barrier_semaphore()
    for axis, me, count in (("dp", d, n_dp), ("kv", z, n_kv), ("tp", t, n_tp)):
        for step in range(1, count):
            pl.semaphore_signal(
                barrier, inc=1, device_id={axis: lax.rem(me + step, count)},
                device_id_type=pl.DeviceIdType.MESH,
            )
    pl.semaphore_wait(barrier, n_dp + n_kv + n_tp - 3)

    owns = (pair_own, query_own, out_own)
    alls = (pair_all, query_all, out_all)

    def first(which, j):
        return remote(
            owns[which].at[d], alls[which].at[z, d], z_send.at[which, j], z_recv.at[which, j],
            "kv", lax.rem(z + j, n_kv),
        )

    def first_in(which, j):
        slot = alls[which].at[lax.rem(z + n_kv - j, n_kv), d]
        return remote(
            slot, slot, z_send.at[which, j], z_recv.at[which, j], "kv", lax.rem(z + j, n_kv)
        )

    def second(which, j, i):
        slot = alls[which].at[lax.rem(z + n_kv - j, n_kv), d]
        return remote(
            slot, slot, d_send.at[which, j, i], d_recv.at[which, j, i],
            "dp", lax.rem(d + i, n_dp),
        )

    def second_in(which, j, i):
        slot = alls[which].at[lax.rem(z + n_kv - j, n_kv), lax.rem(d + n_dp - i, n_dp)]
        return remote(
            slot, slot, d_send.at[which, j, i], d_recv.at[which, j, i],
            "dp", lax.rem(d + i, n_dp),
        )

    def pass_on(which):
        for j in range(1, n_kv):
            first_in(which, j).wait_recv()
            for i in range(1, n_dp):
                second(which, j, i).start()

    def take(which, j):
        if j:
            for i in range(1, n_dp):
                second_in(which, j, i).wait_recv()

    def whole(which, j):
        block = owns[which][...] if j == 0 else alls[which][lax.rem(z + n_kv - j, n_kv)]
        return block.reshape(block.shape[0] * block.shape[1], block.shape[2])

    def token_part(j):
        start = pl.multiple_of(lax.rem(z + n_kv - j, n_kv) * depth, depth)
        return tokens[:, pl.ds(start, depth)]

    for which in (0, 1):
        for j in range(1, n_kv):
            first(which, j).start()
    pass_on(0)
    token_copy.wait()

    total = jnp.dot(token_part(0), whole(0, 0), preferred_element_type=jnp.float32)
    for j in range(1, n_kv):
        take(0, j)
        total += jnp.dot(token_part(j), whole(0, j), preferred_element_type=jnp.float32)
    mine = kv_all.at[pl.ds(z * blocks, blocks)]
    mine[...] = total.astype(jnp.bfloat16).reshape(blocks, BLOCK_LENGTH, LANES)

    def kv_out(j):
        return remote(mine, mine, kv_send.at[j], kv_recv.at[j], "kv", lax.rem(z + j, n_kv))

    def kv_in(j):
        slot = kv_all.at[pl.ds(lax.rem(z + n_kv - j, n_kv) * blocks, blocks)]
        return remote(slot, slot, kv_send.at[j], kv_recv.at[j], "kv", lax.rem(z + j, n_kv))

    for j in range(1, n_kv):
        kv_out(j).start()
    for j in range(1, n_kv):
        first(2, j).start()
    pass_on(1)

    query_sum[...] = jnp.dot(token_part(0), whole(1, 0), preferred_element_type=jnp.float32)
    for j in range(1, n_kv):
        take(1, j)
        query_sum[...] += jnp.dot(token_part(j), whole(1, j), preferred_element_type=jnp.float32)
    query_rows[...] = query_sum[...].astype(jnp.bfloat16) * jnp.bfloat16(HEAD_WIDTH ** (-0.5))

    pass_on(2)
    for j in range(1, n_kv):
        kv_in(j).wait_recv()

    swap = (
        lax.rem(lax.broadcasted_iota(jnp.int32, (LANES, LANES), 0) + HEAD_WIDTH, LANES)
        == lax.broadcasted_iota(jnp.int32, (LANES, LANES), 1)
    ).astype(jnp.float32).astype(jnp.bfloat16)
    for j in range(n_kv):
        part = kv_all[pl.ds(j * blocks, blocks)].reshape(rows, LANES)
        turned = jnp.dot(part, swap, preferred_element_type=jnp.float32)
        vk_all[pl.ds(j * blocks, blocks)] = turned.astype(jnp.bfloat16).reshape(
            blocks, BLOCK_LENGTH, LANES
        )

    picks = chosen.shape[1]
    pairs = query_rows.shape[1] // LANES

    def attend(b, carry):
        lane = lax.broadcasted_iota(jnp.int32, (BLOCK_LENGTH, LANES), 1)
        row = lax.broadcasted_iota(jnp.int32, (BLOCK_LENGTH, LANES), 0)
        low = (lane < HEAD_WIDTH).astype(jnp.float32)
        names = [chosen[b, s] for s in range(picks)]
        offs = [jnp.where(name >= 0, 0.0, HIDDEN) for name in names]
        bias = []
        for s in range(0, picks, 2):
            tile = jnp.where(lane < HEAD_WIDTH, offs[s], offs[s + 1])
            if s == 0:
                tile = jnp.where((lane < HEAD_WIDTH) & (lane > row), HIDDEN, tile)
            bias.append(tile)
        bias = jnp.concatenate(bias, axis=1)
        safe = [jnp.maximum(name, 0) for name in names]
        kv = jnp.concatenate([kv_all[g] for g in safe], axis=0)
        vk = jnp.concatenate([vk_all[g] for g in safe], axis=0)
        at = pl.ds(pl.multiple_of(b * BLOCK_LENGTH, BLOCK_LENGTH), BLOCK_LENGTH)
        query = query_rows[at, :]
        stacked = jnp.concatenate(
            [query[:, p * LANES : (p + 1) * LANES] for p in range(pairs)], axis=0
        )
        keep = jnp.concatenate([low] * pairs, axis=0)
        outs = []
        for side in range(2):
            mask = keep if side == 0 else 1.0 - keep
            masked = stacked * mask.astype(jnp.bfloat16)
            keys, values = (kv, vk) if side == 0 else (vk, kv)
            scores = lax.dot_general(
                masked, keys, (((1,), (1,)), ((), ())), preferred_element_type=jnp.float32
            )
            scores = scores.reshape(pairs, BLOCK_LENGTH, picks * BLOCK_LENGTH) + bias[None]
            top = jnp.max(scores, axis=2, keepdims=True)
            expon = jnp.exp(scores - top)
            inverse = 1.0 / jnp.sum(expon, axis=2, keepdims=True)
            probs = (expon * inverse).astype(jnp.bfloat16)
            probs = probs.reshape(pairs * BLOCK_LENGTH, picks * BLOCK_LENGTH)
            outs.append(jnp.dot(probs, values, preferred_element_type=jnp.float32))
        joined = jnp.where(keep > 0.5, outs[0], outs[1]).astype(jnp.bfloat16)
        for p in range(pairs):
            attended[at, p * LANES : (p + 1) * LANES] = joined[
                p * BLOCK_LENGTH : (p + 1) * BLOCK_LENGTH
            ]
        return carry

    lax.fori_loop(0, blocks, attend, 0)

    peer = lax.rem(t + 1, n_tp)
    other_rows = attended[pl.ds(pl.multiple_of(peer * half, half), half), :]
    own_rows = attended[pl.ds(pl.multiple_of(t * half, half), half), :]

    def swap_half(j):
        slot = lax.rem(z + n_kv - j, n_kv)
        return remote(
            leaving.at[slot], arriving.at[slot], t_send.at[j], t_recv.at[j], "tp", peer
        )

    for j in range(n_kv):
        take(2, j)
        weight = whole(2, j)
        slot = lax.rem(z + n_kv - j, n_kv)
        leaving[slot] = jnp.dot(
            other_rows, weight, preferred_element_type=jnp.float32
        ).astype(jnp.bfloat16)
        swap_half(j).start()
        kept[slot] = jnp.dot(own_rows, weight, preferred_element_type=jnp.float32)

    square = jnp.zeros((half, 1), jnp.float32)
    for j in range(n_kv):
        slot = lax.rem(z + n_kv - j, n_kv)
        swap_half(j).wait_recv()
        mixed = kept[slot] + arriving[slot].astype(jnp.float32)
        kept[slot] = mixed
        square += jnp.sum(mixed * mixed, axis=1, keepdims=True)
    scale = lax.rsqrt(square * (1.0 / width) + 1e-06)
    for j in range(n_kv):
        columns = slice(j * depth, (j + 1) * depth)
        result[:, columns] = (kept[j] * scale * gain[:, columns]).astype(jnp.bfloat16)

    for which in range(3):
        for j in range(1, n_kv):
            first(which, j).wait_send()
            for i in range(1, n_dp):
                second(which, j, i).wait_send()
    for j in range(1, n_kv):
        kv_out(j).wait_send()
    for j in range(n_kv):
        swap_half(j).wait_send()


def per_device_fused(
    n_dp, n_kv, n_tp,
    tokens, chosen, query_weight, key_matrix, value_matrix, out_weight, out_gain,
):
    rows, width = tokens.shape
    depth, columns = query_weight.shape
    blocks = rows // BLOCK_LENGTH
    pair = jnp.concatenate([key_matrix, value_matrix], axis=1)
    cut = lambda w: w.reshape(n_dp, w.shape[0] // n_dp, w.shape[1])
    pair, query, out = cut(pair), cut(query_weight), cut(out_weight)
    bf16, f32 = jnp.bfloat16, jnp.float32
    vmem = pl.BlockSpec(memory_space=pltpu.VMEM)
    dma = pltpu.SemaphoreType.DMA
    return pl.pallas_call(
        functools.partial(fused, n_dp, n_kv, n_tp),
        out_shape=jax.ShapeDtypeStruct((rows // n_tp, width), bf16),
        in_specs=[
            pl.BlockSpec(memory_space=pltpu.SMEM),
            pl.BlockSpec(memory_space=pl.ANY),
            vmem, vmem, vmem, vmem,
        ],
        out_specs=vmem,
        scratch_shapes=[
            pltpu.VMEM((rows, width), bf16),
            pltpu.VMEM((n_kv,) + pair.shape, bf16),
            pltpu.VMEM((n_kv,) + query.shape, bf16),
            pltpu.VMEM((n_kv,) + out.shape, bf16),
            pltpu.VMEM((n_kv * blocks, BLOCK_LENGTH, LANES), bf16),
            pltpu.VMEM((n_kv * blocks, BLOCK_LENGTH, LANES), bf16),
            pltpu.VMEM((rows, columns), f32),
            pltpu.VMEM((rows, columns), bf16),
            pltpu.VMEM((rows, columns), bf16),
            pltpu.VMEM((n_kv, rows // n_tp, width // n_kv), bf16),
            pltpu.VMEM((n_kv, rows // n_tp, width // n_kv), bf16),
            pltpu.VMEM((n_kv, rows // n_tp, width // n_kv), f32),
            dma, dma((3, n_kv)), dma((3, n_kv)), dma((3, n_kv, n_dp)), dma((3, n_kv, n_dp)),
            dma((n_kv,)), dma((n_kv,)), dma((n_kv,)), dma((n_kv,)),
        ],
        compiler_params=pltpu.CompilerParams(
            collective_id=0, has_side_effects=True, vmem_limit_bytes=60 * 1024 * 1024
        ),
    )(chosen, tokens, pair, query, out, out_gain.reshape(1, width))


def per_device(tokens, chosen, query_weight, key_matrix, value_matrix, out_weight, out_gain):
    tok_rows = tokens.shape[0]
    blocks = tok_rows // BLOCK_LENGTH
    device = lax.axis_index("kv")
    kv_count = lax.axis_size("kv")
    whole_query, whole_key, whole_value = (
        lax.all_gather(query_weight, "kv", axis=0, tiled=True),
        lax.all_gather(key_matrix, "kv", axis=0, tiled=True),
        lax.all_gather(value_matrix, "kv", axis=0, tiled=True),
    )
    query_rows = jnp.dot(tokens, whole_query, preferred_element_type=jnp.float32).astype(
        jnp.bfloat16
    )
    key_rows = jnp.dot(tokens, whole_key, preferred_element_type=jnp.float32).astype(jnp.bfloat16)
    value_rows = jnp.dot(tokens, whole_value, preferred_element_type=jnp.float32).astype(
        jnp.bfloat16
    )
    paired = jnp.concatenate([key_rows, value_rows], axis=1)
    pair_width = paired.shape[1]
    safe_ids = jnp.maximum(chosen, 0)
    everyone = lax.all_gather(paired, "kv", axis=0, tiled=True).reshape(
        kv_count * blocks, BLOCK_LENGTH, pair_width
    )
    picked = jnp.take(everyone, safe_ids, axis=0)
    head_count = query_rows.shape[1] // HEAD_WIDTH
    grouped = query_rows.reshape(blocks, BLOCK_LENGTH, head_count, HEAD_WIDTH)
    offsets = jnp.arange(BLOCK_LENGTH, dtype=jnp.int32)
    query_pos = (device * blocks + jnp.arange(blocks, dtype=jnp.int32))[
        :, None
    ] * BLOCK_LENGTH + offsets[None, :]
    key_pos = safe_ids[:, :, None] * BLOCK_LENGTH + offsets[None, None, :]
    visible = (chosen >= 0)[:, None, :, None] & (
        key_pos[:, None, :, :] <= query_pos[:, :, None, None]
    )

    def attend_block(inputs):
        query_block, pair_block, seen = inputs
        block_keys = pair_block[..., :HEAD_WIDTH]
        block_values = pair_block[..., HEAD_WIDTH:]
        scores = jnp.einsum(
            "qgd,skd->gqsk", query_block, block_keys, preferred_element_type=jnp.float32
        ) * HEAD_WIDTH ** (-0.5)
        scores = jnp.where(seen[None], scores, -1e30)
        row_max = jnp.max(scores, axis=(2, 3), keepdims=True)
        expon = jnp.exp(scores - row_max)
        row_sum = jnp.sum(expon, axis=(2, 3), keepdims=True)
        weights_bf = (expon / row_sum).astype(jnp.bfloat16)
        result = jnp.einsum(
            "gqsk,skd->qgd", weights_bf, block_values, preferred_element_type=jnp.float32
        )
        return result.astype(jnp.bfloat16)

    attended = lax.map(attend_block, (grouped, picked, visible))
    attended = attended.reshape(tok_rows, head_count * HEAD_WIDTH)
    whole_out = lax.all_gather(out_weight, "kv", axis=1, tiled=True)
    mixed = lax.psum_scatter(
        jnp.dot(attended, whole_out, preferred_element_type=jnp.float32).astype(jnp.bfloat16),
        "tp",
        scatter_dimension=0,
        tiled=True,
    ).astype(jnp.float32)
    normed = mixed * lax.rsqrt(jnp.mean(mixed * mixed, axis=-1, keepdims=True) + 1e-06) * out_gain
    return normed.astype(jnp.bfloat16)


def solution(mesh):
    placed = (
        P(("dp", "kv"), None),
        P(("dp", "kv"), None),
        P("kv", "tp"),
        P("kv", "tp"),
        P("kv", "tp"),
        P("tp", "kv"),
        P(),
    )
    n_dp, n_kv, n_tp = (mesh.shape[name] for name in ("dp", "kv", "tp"))

    def body(tokens, chosen, query_weight, key_matrix, value_matrix, out_weight, out_gain):
        args = (tokens, chosen, query_weight, key_matrix, value_matrix, out_weight, out_gain)
        depth, columns = query_weight.shape
        whole_tiles = (
            depth % (16 * n_dp) == 0
            and out_weight.shape[0] % (16 * n_dp) == 0
            and out_weight.shape[1] % LANES == 0
            and depth % LANES == 0
            and columns % LANES == 0
            and key_matrix.shape[1] == HEAD_WIDTH
            and chosen.shape[1] % 2 == 0
            and n_tp == 2
        )
        if whole_tiles:
            return per_device_fused(n_dp, n_kv, n_tp, *args)
        return per_device(*args)

    return jax.shard_map(
        body,
        mesh=mesh,
        in_specs=placed,
        out_specs=P(("dp", "kv", "tp"), None),
        check_vma=False,
    )
```

```python
import functools

import jax
import jax.numpy as jnp
from jax import lax
from jax.experimental import pallas as pl
from jax.experimental.pallas import tpu as pltpu
from jax.sharding import PartitionSpec as P

HEAD_WIDTH = 64
BLOCK_LENGTH = 64
LANES = 2 * HEAD_WIDTH
HIDDEN = -1e30


def remote(src, dst, send, recv, axis, peer):
    return pltpu.make_async_remote_copy(
        src_ref=src,
        dst_ref=dst,
        send_sem=send,
        recv_sem=recv,
        device_id={axis: peer},
        device_id_type=pl.DeviceIdType.MESH,
    )


def fused(
    n_dp, n_kv, n_tp,
    chosen_hbm, tokens_hbm, key_hbm, value_hbm, query_hbm, out_hbm, gain_hbm, result,
    chosen, gain, tokens, pair_own, query_own, out_own, pair_all, query_all, out_all, kv_all, vk_all, query_sum, query_rows, attended,
    leaving, arriving, kept,
    load_sem, z_send, z_recv, d_send, d_recv, kv_send, kv_recv, t_send, t_recv,
):
    d, z, t = lax.axis_index("dp"), lax.axis_index("kv"), lax.axis_index("tp")
    rows, width = tokens.shape
    blocks = rows // BLOCK_LENGTH
    depth = width // n_kv
    half = rows // n_tp
    cut = depth // n_dp
    loads = [
        pltpu.make_async_copy(source, target, load_sem.at[k])
        for k, (source, target) in enumerate(
            ((query_hbm, query_own), (tokens_hbm, tokens), (out_hbm, out_own),
             (gain_hbm, gain), (chosen_hbm, chosen))
        )
    ]
    pair_loads = [
        pltpu.make_async_copy(
            source.at[:, k * cut : (k + 1) * cut],
            pair_own.at[k, side * HEAD_WIDTH : (side + 1) * HEAD_WIDTH],
            load_sem.at[5 + k * 2 + side],
        )
        for k in range(n_dp)
        for side, source in enumerate((key_hbm, value_hbm))
    ]
    for load in pair_loads + loads:
        load.start()

    barrier = pltpu.get_barrier_semaphore()
    for axis, me, count in (("dp", d, n_dp), ("kv", z, n_kv), ("tp", t, n_tp)):
        for step in range(1, count):
            pl.semaphore_signal(
                barrier, inc=1, device_id={axis: lax.rem(me + step, count)},
                device_id_type=pl.DeviceIdType.MESH,
            )
    pl.semaphore_wait(barrier, n_dp + n_kv + n_tp - 3)

    owns = (pair_own, query_own, out_own)
    alls = (pair_all, query_all, out_all)

    def first(which, j):
        return remote(
            owns[which].at[d], alls[which].at[z, d], z_send.at[which, j], z_recv.at[which, j],
            "kv", lax.rem(z + j, n_kv),
        )

    def first_in(which, j):
        slot = alls[which].at[lax.rem(z + n_kv - j, n_kv), d]
        return remote(
            slot, slot, z_send.at[which, j], z_recv.at[which, j], "kv", lax.rem(z + j, n_kv)
        )

    def second(which, j, i):
        slot = alls[which].at[lax.rem(z + n_kv - j, n_kv), d]
        return remote(
            slot, slot, d_send.at[which, j, i], d_recv.at[which, j, i],
            "dp", lax.rem(d + i, n_dp),
        )

    def second_in(which, j, i):
        slot = alls[which].at[lax.rem(z + n_kv - j, n_kv), lax.rem(d + n_dp - i, n_dp)]
        return remote(
            slot, slot, d_send.at[which, j, i], d_recv.at[which, j, i],
            "dp", lax.rem(d + i, n_dp),
        )

    def pass_on(which, j):
        first_in(which, j).wait_recv()
        for i in range(1, n_dp):
            second(which, j, i).start()

    def take(which, j):
        if j:
            for i in range(1, n_dp):
                second_in(which, j, i).wait_recv()

    def whole(which, j):
        block = owns[which][...] if j == 0 else alls[which][lax.rem(z + n_kv - j, n_kv)]
        return block.reshape(block.shape[0] * block.shape[1], block.shape[2])

    def token_part(j):
        start = pl.multiple_of(lax.rem(z + n_kv - j, n_kv) * depth, depth)
        return tokens[:, pl.ds(start, depth)]

    for which in (0, 1):
        for load in (pair_loads, loads[:1])[which]:
            load.wait()
        for j in range(1, n_kv):
            first(which, j).start()
    for j in range(1, n_kv):
        pass_on(0, j)
    if n_kv > 1:
        pass_on(1, 1)
    for load in loads[1:]:
        load.wait()

    def pair_part(j):
        block = pair_own[...] if j == 0 else pair_all[lax.rem(z + n_kv - j, n_kv)]
        block = jnp.concatenate([block[k] for k in range(n_dp)], axis=1)
        return lax.dot_general(
            token_part(j), block, (((1,), (1,)), ((), ())), preferred_element_type=jnp.float32
        )

    total = pair_part(0)
    for j in range(1, n_kv):
        take(0, j)
        total += pair_part(j)
    mine = kv_all.at[pl.ds(z * blocks, blocks)]
    mine[...] = total.astype(jnp.bfloat16).reshape(blocks, BLOCK_LENGTH, LANES)

    def kv_out(j):
        return remote(mine, mine, kv_send.at[j], kv_recv.at[j], "kv", lax.rem(z + j, n_kv))

    def kv_in(j):
        slot = kv_all.at[pl.ds(lax.rem(z + n_kv - j, n_kv) * blocks, blocks)]
        return remote(slot, slot, kv_send.at[j], kv_recv.at[j], "kv", lax.rem(z + j, n_kv))

    for j in range(1, n_kv):
        kv_out(j).start()
    for j in range(1, n_kv):
        first(2, j).start()
    for j in range(2, n_kv):
        pass_on(1, j)

    query_sum[...] = jnp.dot(token_part(0), whole(1, 0), preferred_element_type=jnp.float32)
    for j in range(1, n_kv):
        take(1, j)
        query_sum[...] += jnp.dot(token_part(j), whole(1, j), preferred_element_type=jnp.float32)
    query_rows[...] = query_sum[...].astype(jnp.bfloat16) * jnp.bfloat16(HEAD_WIDTH ** (-0.5))

    for j in range(1, n_kv):
        kv_in(j).wait_recv()

    swap = (
        lax.rem(lax.broadcasted_iota(jnp.int32, (LANES, LANES), 0) + HEAD_WIDTH, LANES)
        == lax.broadcasted_iota(jnp.int32, (LANES, LANES), 1)
    ).astype(jnp.float32).astype(jnp.bfloat16)
    for j in range(n_kv):
        part = kv_all[pl.ds(j * blocks, blocks)].reshape(rows, LANES)
        turned = jnp.dot(part, swap, preferred_element_type=jnp.float32)
        vk_all[pl.ds(j * blocks, blocks)] = turned.astype(jnp.bfloat16).reshape(
            blocks, BLOCK_LENGTH, LANES
        )

    picks = chosen.shape[1]
    pairs = query_rows.shape[1] // LANES

    def attend(b, carry):
        for j in range(1, n_kv):

            @pl.when(b == min(2 * j, blocks - 1))
            def _(j=j):
                pass_on(2, j)

        lane = lax.broadcasted_iota(jnp.int32, (BLOCK_LENGTH, LANES), 1)
        row = lax.broadcasted_iota(jnp.int32, (BLOCK_LENGTH, LANES), 0)
        low = (lane < HEAD_WIDTH).astype(jnp.float32)
        names = [chosen[b, s] for s in range(picks)]
        offs = [jnp.where(name >= 0, 0.0, HIDDEN) for name in names]
        bias = []
        for s in range(0, picks, 2):
            tile = jnp.where(lane < HEAD_WIDTH, offs[s], offs[s + 1])
            if s == 0:
                tile = jnp.where((lane < HEAD_WIDTH) & (lane > row), HIDDEN, tile)
            bias.append(tile)
        bias = jnp.concatenate(bias, axis=1)
        safe = [jnp.maximum(name, 0) for name in names]
        kv = jnp.concatenate([kv_all[g] for g in safe], axis=0)
        vk = jnp.concatenate([vk_all[g] for g in safe], axis=0)
        at = pl.ds(pl.multiple_of(b * BLOCK_LENGTH, BLOCK_LENGTH), BLOCK_LENGTH)
        query = query_rows[at, :]
        stacked = jnp.concatenate(
            [query[:, p * LANES : (p + 1) * LANES] for p in range(pairs)], axis=0
        )
        keep = jnp.concatenate([low] * pairs, axis=0)
        outs = []
        for side in range(2):
            mask = keep if side == 0 else 1.0 - keep
            masked = stacked * mask.astype(jnp.bfloat16)
            keys, values = (kv, vk) if side == 0 else (vk, kv)
            scores = lax.dot_general(
                masked, keys, (((1,), (1,)), ((), ())), preferred_element_type=jnp.float32
            )
            scores = scores.reshape(pairs, BLOCK_LENGTH, picks * BLOCK_LENGTH) + bias[None]
            top = jnp.max(scores, axis=2, keepdims=True)
            expon = jnp.exp(scores - top)
            inverse = 1.0 / jnp.sum(expon, axis=2, keepdims=True)
            probs = expon.astype(jnp.bfloat16)
            probs = probs.reshape(pairs * BLOCK_LENGTH, picks * BLOCK_LENGTH)
            out = jnp.dot(probs, values, preferred_element_type=jnp.float32)
            outs.append(out * inverse.reshape(pairs * BLOCK_LENGTH, 1))
        joined = jnp.where(keep > 0.5, outs[0], outs[1]).astype(jnp.bfloat16)
        for p in range(pairs):
            attended[at, p * LANES : (p + 1) * LANES] = joined[
                p * BLOCK_LENGTH : (p + 1) * BLOCK_LENGTH
            ]
        return carry

    lax.fori_loop(0, blocks, attend, 0)

    peer = lax.rem(t + 1, n_tp)
    other_rows = attended[pl.ds(pl.multiple_of(peer * half, half), half), :]
    own_rows = attended[pl.ds(pl.multiple_of(t * half, half), half), :]

    def swap_half(j):
        slot = lax.rem(z + n_kv - j, n_kv)
        return remote(
            leaving.at[slot], arriving.at[slot], t_send.at[j], t_recv.at[j], "tp", peer
        )

    for j in range(n_kv):
        take(2, j)
        weight = whole(2, j)
        slot = lax.rem(z + n_kv - j, n_kv)
        leaving[slot] = jnp.dot(
            other_rows, weight, preferred_element_type=jnp.float32
        ).astype(jnp.bfloat16)
        swap_half(j).start()
        kept[slot] = jnp.dot(own_rows, weight, preferred_element_type=jnp.float32)

    square = jnp.zeros((half, 1), jnp.float32)
    for j in range(n_kv):
        slot = lax.rem(z + n_kv - j, n_kv)
        swap_half(j).wait_recv()
        mixed = kept[slot] + arriving[slot].astype(jnp.float32)
        kept[slot] = mixed
        square += jnp.sum(mixed * mixed, axis=1, keepdims=True)
    scale = lax.rsqrt(square * (1.0 / width) + 1e-06)
    for j in range(n_kv):
        columns = slice(j * depth, (j + 1) * depth)
        result[:, columns] = (kept[j] * scale * gain[:, columns]).astype(jnp.bfloat16)

    for which in range(3):
        for j in range(1, n_kv):
            first(which, j).wait_send()
            for i in range(1, n_dp):
                second(which, j, i).wait_send()
    for j in range(1, n_kv):
        kv_out(j).wait_send()
    for j in range(n_kv):
        swap_half(j).wait_send()


def per_device_fused(
    n_dp, n_kv, n_tp,
    tokens, chosen, query_weight, key_matrix, value_matrix, out_weight, out_gain,
):
    rows, width = tokens.shape
    depth, columns = query_weight.shape
    blocks = rows // BLOCK_LENGTH
    cut = lambda w: w.reshape(n_dp, w.shape[0] // n_dp, w.shape[1])
    query, out = cut(query_weight), cut(out_weight)
    pair = jax.ShapeDtypeStruct((n_dp, LANES, depth // n_dp), jnp.bfloat16)
    bf16, f32 = jnp.bfloat16, jnp.float32
    vmem = pl.BlockSpec(memory_space=pltpu.VMEM)
    off_core = pl.BlockSpec(memory_space=pltpu.HBM)
    dma = pltpu.SemaphoreType.DMA
    return pl.pallas_call(
        functools.partial(fused, n_dp, n_kv, n_tp),
        out_shape=jax.ShapeDtypeStruct((rows // n_tp, width), bf16),
        in_specs=[
            off_core, off_core, off_core, off_core, off_core, off_core, off_core,
        ],
        out_specs=vmem,
        scratch_shapes=[
            pltpu.SMEM((blocks, chosen.shape[1]), jnp.int32),
            pltpu.VMEM((1, width), f32),
            pltpu.VMEM((rows, width), bf16),
            pltpu.VMEM(pair.shape, bf16),
            pltpu.VMEM(query.shape, bf16),
            pltpu.VMEM(out.shape, bf16),
            pltpu.VMEM((n_kv,) + pair.shape, bf16),
            pltpu.VMEM((n_kv,) + query.shape, bf16),
            pltpu.VMEM((n_kv,) + out.shape, bf16),
            pltpu.VMEM((n_kv * blocks, BLOCK_LENGTH, LANES), bf16),
            pltpu.VMEM((n_kv * blocks, BLOCK_LENGTH, LANES), bf16),
            pltpu.VMEM((rows, columns), f32),
            pltpu.VMEM((rows, columns), bf16),
            pltpu.VMEM((rows, columns), bf16),
            pltpu.VMEM((n_kv, rows // n_tp, width // n_kv), bf16),
            pltpu.VMEM((n_kv, rows // n_tp, width // n_kv), bf16),
            pltpu.VMEM((n_kv, rows // n_tp, width // n_kv), f32),
            dma((5 + 2 * n_dp,)), dma((3, n_kv)), dma((3, n_kv)), dma((3, n_kv, n_dp)), dma((3, n_kv, n_dp)),
            dma((n_kv,)), dma((n_kv,)), dma((n_kv,)), dma((n_kv,)),
        ],
        compiler_params=pltpu.CompilerParams(
            collective_id=0, has_side_effects=True, vmem_limit_bytes=54 * 1024 * 1024
        ),
    )(chosen, tokens, key_matrix.T, value_matrix.T, query, out, out_gain.reshape(1, width))


def per_device(tokens, chosen, query_weight, key_matrix, value_matrix, out_weight, out_gain):
    tok_rows = tokens.shape[0]
    blocks = tok_rows // BLOCK_LENGTH
    device = lax.axis_index("kv")
    kv_count = lax.axis_size("kv")
    whole_query, whole_key, whole_value = (
        lax.all_gather(query_weight, "kv", axis=0, tiled=True),
        lax.all_gather(key_matrix, "kv", axis=0, tiled=True),
        lax.all_gather(value_matrix, "kv", axis=0, tiled=True),
    )
    query_rows = jnp.dot(tokens, whole_query, preferred_element_type=jnp.float32).astype(
        jnp.bfloat16
    )
    key_rows = jnp.dot(tokens, whole_key, preferred_element_type=jnp.float32).astype(jnp.bfloat16)
    value_rows = jnp.dot(tokens, whole_value, preferred_element_type=jnp.float32).astype(
        jnp.bfloat16
    )
    paired = jnp.concatenate([key_rows, value_rows], axis=1)
    pair_width = paired.shape[1]
    safe_ids = jnp.maximum(chosen, 0)
    everyone = lax.all_gather(paired, "kv", axis=0, tiled=True).reshape(
        kv_count * blocks, BLOCK_LENGTH, pair_width
    )
    picked = jnp.take(everyone, safe_ids, axis=0)
    head_count = query_rows.shape[1] // HEAD_WIDTH
    grouped = query_rows.reshape(blocks, BLOCK_LENGTH, head_count, HEAD_WIDTH)
    offsets = jnp.arange(BLOCK_LENGTH, dtype=jnp.int32)
    query_pos = (device * blocks + jnp.arange(blocks, dtype=jnp.int32))[
        :, None
    ] * BLOCK_LENGTH + offsets[None, :]
    key_pos = safe_ids[:, :, None] * BLOCK_LENGTH + offsets[None, None, :]
    visible = (chosen >= 0)[:, None, :, None] & (
        key_pos[:, None, :, :] <= query_pos[:, :, None, None]
    )

    def attend_block(inputs):
        query_block, pair_block, seen = inputs
        block_keys = pair_block[..., :HEAD_WIDTH]
        block_values = pair_block[..., HEAD_WIDTH:]
        scores = jnp.einsum(
            "qgd,skd->gqsk", query_block, block_keys, preferred_element_type=jnp.float32
        ) * HEAD_WIDTH ** (-0.5)
        scores = jnp.where(seen[None], scores, -1e30)
        row_max = jnp.max(scores, axis=(2, 3), keepdims=True)
        expon = jnp.exp(scores - row_max)
        row_sum = jnp.sum(expon, axis=(2, 3), keepdims=True)
        weights_bf = (expon / row_sum).astype(jnp.bfloat16)
        result = jnp.einsum(
            "gqsk,skd->qgd", weights_bf, block_values, preferred_element_type=jnp.float32
        )
        return result.astype(jnp.bfloat16)

    attended = lax.map(attend_block, (grouped, picked, visible))
    attended = attended.reshape(tok_rows, head_count * HEAD_WIDTH)
    whole_out = lax.all_gather(out_weight, "kv", axis=1, tiled=True)
    mixed = lax.psum_scatter(
        jnp.dot(attended, whole_out, preferred_element_type=jnp.float32).astype(jnp.bfloat16),
        "tp",
        scatter_dimension=0,
        tiled=True,
    ).astype(jnp.float32)
    normed = mixed * lax.rsqrt(jnp.mean(mixed * mixed, axis=-1, keepdims=True) + 1e-06) * out_gain
    return normed.astype(jnp.bfloat16)


def solution(mesh):
    placed = (
        P(("dp", "kv"), None),
        P(("dp", "kv"), None),
        P("kv", "tp"),
        P("kv", "tp"),
        P("kv", "tp"),
        P("tp", "kv"),
        P(),
    )
    n_dp, n_kv, n_tp = (mesh.shape[name] for name in ("dp", "kv", "tp"))

    def body(tokens, chosen, query_weight, key_matrix, value_matrix, out_weight, out_gain):
        args = (tokens, chosen, query_weight, key_matrix, value_matrix, out_weight, out_gain)
        depth, columns = query_weight.shape
        whole_tiles = (
            depth % (LANES * n_dp) == 0
            and out_weight.shape[0] % (16 * n_dp) == 0
            and out_weight.shape[1] % LANES == 0
            and columns % LANES == 0
            and key_matrix.shape[1] == HEAD_WIDTH
            and chosen.shape[1] % 2 == 0
            and n_tp == 2
        )
        if whole_tiles:
            return per_device_fused(n_dp, n_kv, n_tp, *args)
        return per_device(*args)

    return jax.shard_map(
        body,
        mesh=mesh,
        in_specs=placed,
        out_specs=P(("dp", "kv", "tp"), None),
        check_vma=False,
    )
```

```python
import functools

import jax
import jax.numpy as jnp
from jax import lax
from jax.experimental import pallas as pl
from jax.experimental.pallas import tpu as pltpu
from jax.sharding import PartitionSpec as P

HEAD_WIDTH = 64
BLOCK_LENGTH = 64
LANES = 2 * HEAD_WIDTH
HIDDEN = -1e30
CAP = 2


def remote(src, dst, send, recv, axis, peer):
    return pltpu.make_async_remote_copy(
        src_ref=src,
        dst_ref=dst,
        send_sem=send,
        recv_sem=recv,
        device_id={axis: peer},
        device_id_type=pl.DeviceIdType.MESH,
    )


def fused(
    n_dp, n_kv, n_tp,
    chosen_hbm, tokens_hbm, key_hbm, value_hbm, query_hbm, out_hbm, gain_hbm, result,
    chosen, gain, tokens, pair_own, query_own, out_own, wanted, asks, packed, kv_own, kv_far,
    pair_all, query_all, out_all, kv_all, vk_all, query_sum, query_rows, attended,
    leaving, arriving, kept,
    load_sem, z_send, z_recv, d_send, d_recv, r_send, r_recv, kv_send, kv_recv, t_send, t_recv, ask_send, ask_recv,
):
    d, z, t = lax.axis_index("dp"), lax.axis_index("kv"), lax.axis_index("tp")
    rows, width = tokens.shape
    blocks = rows // BLOCK_LENGTH
    depth = width // n_kv
    half = rows // n_tp
    cut = depth // n_dp
    loads = [
        pltpu.make_async_copy(source, target, load_sem.at[k])
        for k, (source, target) in enumerate(
            ((query_hbm, query_own), (tokens_hbm, tokens), (out_hbm, out_own),
             (gain_hbm, gain), (chosen_hbm, wanted), (chosen_hbm, chosen))
        )
    ]
    pair_loads = [
        pltpu.make_async_copy(
            source.at[:, k * cut : (k + 1) * cut],
            pair_own.at[k, side * HEAD_WIDTH : (side + 1) * HEAD_WIDTH],
            load_sem.at[6 + k * 2 + side],
        )
        for k in range(n_dp)
        for side, source in enumerate((key_hbm, value_hbm))
    ]
    for load in pair_loads + loads:
        load.start()

    barrier = pltpu.get_barrier_semaphore()
    for axis, me, count in (("dp", d, n_dp), ("kv", z, n_kv), ("tp", t, n_tp)):
        for step in range(1, count):
            pl.semaphore_signal(
                barrier, inc=1, device_id={axis: lax.rem(me + step, count)},
                device_id_type=pl.DeviceIdType.MESH,
            )
    pl.semaphore_wait(barrier, n_dp + n_kv + n_tp - 3)

    owns = (pair_own, query_own, out_own)
    alls = (pair_all, query_all, out_all)

    def first(which, j):
        return remote(
            owns[which].at[d], alls[which].at[z, d], z_send.at[which, j], z_recv.at[which, j],
            "kv", lax.rem(z + j, n_kv),
        )

    def first_in(which, j):
        slot = alls[which].at[lax.rem(z + n_kv - j, n_kv), d]
        return remote(
            slot, slot, z_send.at[which, j], z_recv.at[which, j], "kv", lax.rem(z + j, n_kv)
        )

    near = (d, d + 1 - 2 * lax.rem(d, 2), lax.rem(d + 2, 4))
    corner = 3 - d

    def second(which, j, k, place=None):
        slot = alls[which].at[lax.rem(z + n_kv - j, n_kv), d if place is None else place]
        return remote(
            slot, slot, d_send.at[which, j, k], d_recv.at[which, j, k], "dp", near[k]
        )

    def halfway(which, j, k, place):
        rows_half = owns[which].shape[1] // 2
        slot = alls[which].at[
            lax.rem(z + n_kv - j, n_kv), place, (k - 1) * rows_half : k * rows_half
        ]
        return remote(
            slot, slot, r_send.at[which, j, k], r_recv.at[which, j, k], "dp", near[3 - k]
        )

    def relay(which, j):
        for k in (1, 2):
            second(which, j, k, near[k]).wait_recv()
            halfway(which, j, k, near[k]).start()

    def pass_on(which, j):
        first_in(which, j).wait_recv()
        for k in (1, 2):
            second(which, j, k).start()

    def take(which, j):
        if j:
            for k in (1, 2):
                halfway(which, j, k, corner).wait_recv()

    def whole(which, j):
        block = owns[which][...] if j == 0 else alls[which][lax.rem(z + n_kv - j, n_kv)]
        return block.reshape(block.shape[0] * block.shape[1], block.shape[2])

    def token_part(j):
        start = pl.multiple_of(lax.rem(z + n_kv - j, n_kv) * depth, depth)
        return tokens[:, pl.ds(start, depth)]

    def ask(j):
        return remote(
            wanted, asks.at[z], ask_send.at[j], ask_recv.at[j], "kv", lax.rem(z + n_kv - j, n_kv)
        )

    def ask_in(j):
        slot = asks.at[lax.rem(z + j, n_kv)]
        return remote(
            slot, slot, ask_send.at[j], ask_recv.at[j], "kv", lax.rem(z + n_kv - j, n_kv)
        )

    loads[4].wait()
    for j in range(1, n_kv):
        ask(j).start()
    for which in (0, 1):
        for load in (pair_loads, loads[:1])[which]:
            load.wait()
        for j in range(1, n_kv):
            first(which, j).start()
    for j in range(1, n_kv):
        pass_on(0, j)
    if n_kv > 1:
        pass_on(1, 1)
    for load in loads[1:4] + loads[5:]:
        load.wait()

    def pair_part(j):
        block = pair_own[...] if j == 0 else pair_all[lax.rem(z + n_kv - j, n_kv)]
        block = jnp.concatenate([block[k] for k in range(n_dp)], axis=1)
        return lax.dot_general(
            token_part(j), block, (((1,), (1,)), ((), ())), preferred_element_type=jnp.float32
        )

    total = pair_part(0)
    for j in range(1, n_kv):
        relay(0, j)
    for j in range(1, n_kv):
        take(0, j)
        total += pair_part(j)
    kv_own[...] = total.astype(jnp.bfloat16).reshape(blocks, BLOCK_LENGTH, LANES)

    def named(rows_of, owner):
        local = rows_of - owner * blocks
        inside = (local >= 0) & (local < blocks)
        return (
            jnp.min(jnp.where(inside, local, blocks - 1)),
            jnp.max(jnp.where(inside, local, 0)),
        )

    def kv_out(j):
        return remote(
            packed.at[j], kv_far.at[pl.ds(z * CAP, CAP)], kv_send.at[j], kv_recv.at[j],
            "kv", lax.rem(z + j, n_kv),
        )

    def kv_in(j):
        slot = kv_far.at[pl.ds(lax.rem(z + n_kv - j, n_kv) * CAP, CAP)]
        return remote(slot, slot, kv_send.at[j], kv_recv.at[j], "kv", lax.rem(z + j, n_kv))

    kv_far[pl.ds(z * CAP, CAP)] = jnp.zeros((CAP, BLOCK_LENGTH, LANES), jnp.bfloat16)
    for j in range(1, n_kv):
        ask_in(j).wait_recv()
        lowest, highest = named(asks[lax.rem(z + j, n_kv)], z)
        packed[j, 0] = kv_own[lowest]
        packed[j, 1] = kv_own[highest]
    firsts = [named(wanted[...], owner)[0] + owner * blocks for owner in range(n_kv)]
    for j in range(1, n_kv):
        kv_out(j).start()
    for j in range(1, n_kv):
        first(2, j).start()
    for j in range(2, n_kv):
        pass_on(1, j)
        relay(1, j - 1)
    if n_kv > 1:
        relay(1, n_kv - 1)

    query_sum[...] = jnp.dot(token_part(0), whole(1, 0), preferred_element_type=jnp.float32)
    for j in range(1, n_kv):
        if j == n_kv - 1:
            pass_on(2, 1)
        take(1, j)
        query_sum[...] += jnp.dot(token_part(j), whole(1, j), preferred_element_type=jnp.float32)
    query_rows[...] = query_sum[...].astype(jnp.bfloat16) * jnp.bfloat16(HEAD_WIDTH ** (-0.5))

    for j in range(1, n_kv):
        kv_in(j).wait_recv()

    swap = (
        lax.rem(lax.broadcasted_iota(jnp.int32, (LANES, LANES), 0) + HEAD_WIDTH, LANES)
        == lax.broadcasted_iota(jnp.int32, (LANES, LANES), 1)
    ).astype(jnp.float32).astype(jnp.bfloat16)
    for source, start in ((kv_far, 0), (kv_own, n_kv * CAP)):
        count = source.shape[0]
        part = source[...]
        turned = jnp.dot(
            part.reshape(count * BLOCK_LENGTH, LANES), swap, preferred_element_type=jnp.float32
        )
        kv_all[start : start + count] = part
        vk_all[start : start + count] = turned.astype(jnp.bfloat16).reshape(part.shape)

    picks = chosen.shape[1]
    pairs = query_rows.shape[1] // LANES

    def attend(b, carry):
        for j in range(1, n_kv):

            @pl.when(b == min(2 * (j - 1), blocks - 1))
            def _(j=j):
                if j < n_kv - 1:
                    pass_on(2, j + 1)

            @pl.when(b == min(2 * j, blocks - 1))
            def _(j=j):
                relay(2, j)

        lane = lax.broadcasted_iota(jnp.int32, (BLOCK_LENGTH, LANES), 1)
        row = lax.broadcasted_iota(jnp.int32, (BLOCK_LENGTH, LANES), 0)
        low = (lane < HEAD_WIDTH).astype(jnp.float32)
        names = [chosen[b, s] for s in range(picks)]
        offs = [jnp.where(name >= 0, 0.0, HIDDEN) for name in names]
        bias = []
        for s in range(0, picks, 2):
            tile = jnp.where(lane < HEAD_WIDTH, offs[s], offs[s + 1])
            if s == 0:
                tile = jnp.where((lane < HEAD_WIDTH) & (lane > row), HIDDEN, tile)
            bias.append(tile)
        bias = jnp.concatenate(bias, axis=1)

        def place(name):
            name = jnp.maximum(name, 0)
            spot = name - z * blocks + n_kv * CAP
            for owner in range(n_kv):
                local = name - owner * blocks
                away = (local >= 0) & (local < blocks) & (z != owner)
                far = owner * CAP + jnp.where(name == firsts[owner], 0, 1)
                spot = jnp.where(away, far, spot)
            return spot

        safe = [jnp.where(name >= 0, place(name), 0) for name in names]
        kv = jnp.concatenate([kv_all[g] for g in safe], axis=0)
        vk = jnp.concatenate([vk_all[g] for g in safe], axis=0)
        at = pl.ds(pl.multiple_of(b * BLOCK_LENGTH, BLOCK_LENGTH), BLOCK_LENGTH)
        query = query_rows[at, :]
        stacked = jnp.concatenate(
            [query[:, p * LANES : (p + 1) * LANES] for p in range(pairs)], axis=0
        )
        keep = jnp.concatenate([low] * pairs, axis=0)
        outs = []
        for side in range(2):
            mask = keep if side == 0 else 1.0 - keep
            masked = stacked * mask.astype(jnp.bfloat16)
            keys, values = (kv, vk) if side == 0 else (vk, kv)
            scores = lax.dot_general(
                masked, keys, (((1,), (1,)), ((), ())), preferred_element_type=jnp.float32
            )
            scores = scores.reshape(pairs, BLOCK_LENGTH, picks * BLOCK_LENGTH) + bias[None]
            top = jnp.max(scores, axis=2, keepdims=True)
            expon = jnp.exp(scores - top)
            inverse = 1.0 / jnp.sum(expon, axis=2, keepdims=True)
            probs = expon.astype(jnp.bfloat16)
            probs = probs.reshape(pairs * BLOCK_LENGTH, picks * BLOCK_LENGTH)
            out = jnp.dot(probs, values, preferred_element_type=jnp.float32)
            outs.append(out * inverse.reshape(pairs * BLOCK_LENGTH, 1))
        joined = jnp.where(keep > 0.5, outs[0], outs[1]).astype(jnp.bfloat16)
        for p in range(pairs):
            attended[at, p * LANES : (p + 1) * LANES] = joined[
                p * BLOCK_LENGTH : (p + 1) * BLOCK_LENGTH
            ]
        return carry

    lax.fori_loop(0, blocks, attend, 0)

    peer = lax.rem(t + 1, n_tp)
    other_rows = attended[pl.ds(pl.multiple_of(peer * half, half), half), :]
    own_rows = attended[pl.ds(pl.multiple_of(t * half, half), half), :]

    def swap_half(j):
        slot = lax.rem(z + n_kv - j, n_kv)
        return remote(
            leaving.at[slot], arriving.at[slot], t_send.at[j], t_recv.at[j], "tp", peer
        )

    for j in range(n_kv):
        take(2, j)
        weight = whole(2, j)
        slot = lax.rem(z + n_kv - j, n_kv)
        leaving[slot] = jnp.dot(
            other_rows, weight, preferred_element_type=jnp.float32
        ).astype(jnp.bfloat16)
        swap_half(j).start()
        kept[slot] = jnp.dot(own_rows, weight, preferred_element_type=jnp.float32)

    square = jnp.zeros((half, 1), jnp.float32)
    for j in range(n_kv):
        slot = lax.rem(z + n_kv - j, n_kv)
        swap_half(j).wait_recv()
        mixed = kept[slot] + arriving[slot].astype(jnp.float32)
        kept[slot] = mixed
        square += jnp.sum(mixed * mixed, axis=1, keepdims=True)
    scale = lax.rsqrt(square * (1.0 / width) + 1e-06)
    for j in range(n_kv):
        columns = slice(j * depth, (j + 1) * depth)
        result[:, columns] = (kept[j] * scale * gain[:, columns]).astype(jnp.bfloat16)

    for which in range(3):
        for j in range(1, n_kv):
            first(which, j).wait_send()
            for k in (1, 2):
                second(which, j, k).wait_send()
                halfway(which, j, k, near[k]).wait_send()
    for j in range(1, n_kv):
        kv_out(j).wait_send()
        ask(j).wait_send()
    for j in range(n_kv):
        swap_half(j).wait_send()


def per_device_fused(
    n_dp, n_kv, n_tp,
    tokens, chosen, query_weight, key_matrix, value_matrix, out_weight, out_gain,
):
    rows, width = tokens.shape
    depth, columns = query_weight.shape
    blocks = rows // BLOCK_LENGTH
    cut = lambda w: w.reshape(n_dp, w.shape[0] // n_dp, w.shape[1])
    query, out = cut(query_weight), cut(out_weight)
    pair = jax.ShapeDtypeStruct((n_dp, LANES, depth // n_dp), jnp.bfloat16)
    bf16, f32 = jnp.bfloat16, jnp.float32
    vmem = pl.BlockSpec(memory_space=pltpu.VMEM)
    off_core = pl.BlockSpec(memory_space=pltpu.HBM)
    dma = pltpu.SemaphoreType.DMA
    return pl.pallas_call(
        functools.partial(fused, n_dp, n_kv, n_tp),
        out_shape=jax.ShapeDtypeStruct((rows // n_tp, width), bf16),
        in_specs=[
            off_core, off_core, off_core, off_core, off_core, off_core, off_core,
        ],
        out_specs=vmem,
        scratch_shapes=[
            pltpu.SMEM((blocks, chosen.shape[1]), jnp.int32),
            pltpu.VMEM((1, width), f32),
            pltpu.VMEM((rows, width), bf16),
            pltpu.VMEM(pair.shape, bf16),
            pltpu.VMEM(query.shape, bf16),
            pltpu.VMEM(out.shape, bf16),
            pltpu.VMEM((blocks, chosen.shape[1]), jnp.int32),
            pltpu.VMEM((n_kv, blocks, chosen.shape[1]), jnp.int32),
            pltpu.VMEM((n_kv, CAP, BLOCK_LENGTH, LANES), bf16),
            pltpu.VMEM((blocks, BLOCK_LENGTH, LANES), bf16),
            pltpu.VMEM((n_kv * CAP, BLOCK_LENGTH, LANES), bf16),
            pltpu.VMEM((n_kv,) + pair.shape, bf16),
            pltpu.VMEM((n_kv,) + query.shape, bf16),
            pltpu.VMEM((n_kv,) + out.shape, bf16),
            pltpu.VMEM((n_kv * CAP + blocks, BLOCK_LENGTH, LANES), bf16),
            pltpu.VMEM((n_kv * CAP + blocks, BLOCK_LENGTH, LANES), bf16),
            pltpu.VMEM((rows, columns), f32),
            pltpu.VMEM((rows, columns), bf16),
            pltpu.VMEM((rows, columns), bf16),
            pltpu.VMEM((n_kv, rows // n_tp, width // n_kv), bf16),
            pltpu.VMEM((n_kv, rows // n_tp, width // n_kv), bf16),
            pltpu.VMEM((n_kv, rows // n_tp, width // n_kv), f32),
            dma((6 + 2 * n_dp,)), dma((3, n_kv)), dma((3, n_kv)), dma((3, n_kv, 3)), dma((3, n_kv, 3)),
            dma((3, n_kv, 3)), dma((3, n_kv, 3)),
            dma((n_kv,)), dma((n_kv,)), dma((n_kv,)), dma((n_kv,)),
            dma((n_kv,)), dma((n_kv,)),
        ],
        compiler_params=pltpu.CompilerParams(
            collective_id=0, has_side_effects=True, vmem_limit_bytes=54 * 1024 * 1024
        ),
    )(chosen, tokens, key_matrix.T, value_matrix.T, query, out, out_gain.reshape(1, width))


def per_device(tokens, chosen, query_weight, key_matrix, value_matrix, out_weight, out_gain):
    tok_rows = tokens.shape[0]
    blocks = tok_rows // BLOCK_LENGTH
    device = lax.axis_index("kv")
    kv_count = lax.axis_size("kv")
    whole_query, whole_key, whole_value = (
        lax.all_gather(query_weight, "kv", axis=0, tiled=True),
        lax.all_gather(key_matrix, "kv", axis=0, tiled=True),
        lax.all_gather(value_matrix, "kv", axis=0, tiled=True),
    )
    query_rows = jnp.dot(tokens, whole_query, preferred_element_type=jnp.float32).astype(
        jnp.bfloat16
    )
    key_rows = jnp.dot(tokens, whole_key, preferred_element_type=jnp.float32).astype(jnp.bfloat16)
    value_rows = jnp.dot(tokens, whole_value, preferred_element_type=jnp.float32).astype(
        jnp.bfloat16
    )
    paired = jnp.concatenate([key_rows, value_rows], axis=1)
    pair_width = paired.shape[1]
    safe_ids = jnp.maximum(chosen, 0)
    everyone = lax.all_gather(paired, "kv", axis=0, tiled=True).reshape(
        kv_count * blocks, BLOCK_LENGTH, pair_width
    )
    picked = jnp.take(everyone, safe_ids, axis=0)
    head_count = query_rows.shape[1] // HEAD_WIDTH
    grouped = query_rows.reshape(blocks, BLOCK_LENGTH, head_count, HEAD_WIDTH)
    offsets = jnp.arange(BLOCK_LENGTH, dtype=jnp.int32)
    query_pos = (device * blocks + jnp.arange(blocks, dtype=jnp.int32))[
        :, None
    ] * BLOCK_LENGTH + offsets[None, :]
    key_pos = safe_ids[:, :, None] * BLOCK_LENGTH + offsets[None, None, :]
    visible = (chosen >= 0)[:, None, :, None] & (
        key_pos[:, None, :, :] <= query_pos[:, :, None, None]
    )

    def attend_block(inputs):
        query_block, pair_block, seen = inputs
        block_keys = pair_block[..., :HEAD_WIDTH]
        block_values = pair_block[..., HEAD_WIDTH:]
        scores = jnp.einsum(
            "qgd,skd->gqsk", query_block, block_keys, preferred_element_type=jnp.float32
        ) * HEAD_WIDTH ** (-0.5)
        scores = jnp.where(seen[None], scores, -1e30)
        row_max = jnp.max(scores, axis=(2, 3), keepdims=True)
        expon = jnp.exp(scores - row_max)
        row_sum = jnp.sum(expon, axis=(2, 3), keepdims=True)
        weights_bf = (expon / row_sum).astype(jnp.bfloat16)
        result = jnp.einsum(
            "gqsk,skd->qgd", weights_bf, block_values, preferred_element_type=jnp.float32
        )
        return result.astype(jnp.bfloat16)

    attended = lax.map(attend_block, (grouped, picked, visible))
    attended = attended.reshape(tok_rows, head_count * HEAD_WIDTH)
    whole_out = lax.all_gather(out_weight, "kv", axis=1, tiled=True)
    mixed = lax.psum_scatter(
        jnp.dot(attended, whole_out, preferred_element_type=jnp.float32).astype(jnp.bfloat16),
        "tp",
        scatter_dimension=0,
        tiled=True,
    ).astype(jnp.float32)
    normed = mixed * lax.rsqrt(jnp.mean(mixed * mixed, axis=-1, keepdims=True) + 1e-06) * out_gain
    return normed.astype(jnp.bfloat16)


def solution(mesh):
    placed = (
        P(("dp", "kv"), None),
        P(("dp", "kv"), None),
        P("kv", "tp"),
        P("kv", "tp"),
        P("kv", "tp"),
        P("tp", "kv"),
        P(),
    )
    n_dp, n_kv, n_tp = (mesh.shape[name] for name in ("dp", "kv", "tp"))

    def body(tokens, chosen, query_weight, key_matrix, value_matrix, out_weight, out_gain):
        args = (tokens, chosen, query_weight, key_matrix, value_matrix, out_weight, out_gain)
        depth, columns = query_weight.shape
        whole_tiles = (
            depth % (LANES * n_dp) == 0
            and out_weight.shape[0] % (16 * n_dp) == 0
            and out_weight.shape[1] % LANES == 0
            and columns % LANES == 0
            and key_matrix.shape[1] == HEAD_WIDTH
            and chosen.shape[1] % 2 == 0
            and n_tp == 2
            and n_dp == 4
        )
        if whole_tiles:
            return per_device_fused(n_dp, n_kv, n_tp, *args)
        return per_device(*args)

    return jax.shard_map(
        body,
        mesh=mesh,
        in_specs=placed,
        out_specs=P(("dp", "kv", "tp"), None),
        check_vma=False,
    )
```

```python
import functools

import jax
import jax.numpy as jnp
from jax import lax
from jax.experimental import pallas as pl
from jax.experimental.pallas import tpu as pltpu
from jax.sharding import PartitionSpec as P

HEAD_WIDTH = 64
BLOCK_LENGTH = 64
LANES = 2 * HEAD_WIDTH
HIDDEN = -1e30
CAP = 2


def remote(src, dst, send, recv, axis, peer):
    return pltpu.make_async_remote_copy(
        src_ref=src,
        dst_ref=dst,
        send_sem=send,
        recv_sem=recv,
        device_id={axis: peer},
        device_id_type=pl.DeviceIdType.MESH,
    )


def fused(
    n_dp, n_kv, n_tp,
    chosen_hbm, tokens_hbm, key_hbm, value_hbm, query_hbm, out_hbm, gain_hbm, result,
    chosen, gain, tokens, pair_own, query_own, out_own, wanted, asks, packed, kv_own, kv_far,
    pair_all, query_all, out_all, kv_all, vk_all, query_sum, query_rows, attended,
    leaving, arriving, kept,
    load_sem, z_send, z_recv, d_send, d_recv, r_send, r_recv, kv_send, kv_recv, t_send, t_recv, ask_send, ask_recv,
):
    d, z, t = lax.axis_index("dp"), lax.axis_index("kv"), lax.axis_index("tp")
    rows, width = tokens.shape
    blocks = rows // BLOCK_LENGTH
    depth = width // n_kv
    half = rows // n_tp
    cut = depth // n_dp
    loads = [
        pltpu.make_async_copy(source, target, load_sem.at[k])
        for k, (source, target) in enumerate(
            ((query_hbm, query_own), (tokens_hbm, tokens), (out_hbm, out_own),
             (gain_hbm, gain), (chosen_hbm, wanted), (chosen_hbm, chosen))
        )
    ]
    pair_loads = [
        pltpu.make_async_copy(
            source.at[:, k * cut : (k + 1) * cut],
            pair_own.at[k, side * HEAD_WIDTH : (side + 1) * HEAD_WIDTH],
            load_sem.at[6 + k * 2 + side],
        )
        for k in range(n_dp)
        for side, source in enumerate((key_hbm, value_hbm))
    ]
    for load in pair_loads + loads:
        load.start()

    barrier = pltpu.get_barrier_semaphore()
    for axis, me, count in (("dp", d, n_dp), ("kv", z, n_kv), ("tp", t, n_tp)):
        for step in range(1, count):
            pl.semaphore_signal(
                barrier, inc=1, device_id={axis: lax.rem(me + step, count)},
                device_id_type=pl.DeviceIdType.MESH,
            )
    pl.semaphore_wait(barrier, n_dp + n_kv + n_tp - 3)

    owns = (pair_own, query_own, out_own)
    alls = (pair_all, query_all, out_all)

    def first(which, j):
        return remote(
            owns[which].at[d], alls[which].at[z, d], z_send.at[which, j], z_recv.at[which, j],
            "kv", lax.rem(z + j, n_kv),
        )

    def first_in(which, j):
        slot = alls[which].at[lax.rem(z + n_kv - j, n_kv), d]
        return remote(
            slot, slot, z_send.at[which, j], z_recv.at[which, j], "kv", lax.rem(z + j, n_kv)
        )

    near = (d, d + 1 - 2 * lax.rem(d, 2), lax.rem(d + 2, 4))
    corner = 3 - d

    def second(which, j, k, place=None):
        slot = alls[which].at[lax.rem(z + n_kv - j, n_kv), d if place is None else place]
        return remote(
            slot, slot, d_send.at[which, j, k], d_recv.at[which, j, k], "dp", near[k]
        )

    def halfway(which, j, k, place):
        rows_half = owns[which].shape[1] // 2
        slot = alls[which].at[
            lax.rem(z + n_kv - j, n_kv), place, (k - 1) * rows_half : k * rows_half
        ]
        return remote(
            slot, slot, r_send.at[which, j, k], r_recv.at[which, j, k], "dp", near[3 - k]
        )

    def relay(which, j):
        for k in (1, 2):
            second(which, j, k, near[k]).wait_recv()
            halfway(which, j, k, near[k]).start()

    def pass_on(which, j):
        first_in(which, j).wait_recv()
        for k in (1, 2):
            second(which, j, k).start()

    def take(which, j):
        if j:
            for k in (1, 2):
                halfway(which, j, k, corner).wait_recv()

    def whole(which, j):
        block = owns[which][...] if j == 0 else alls[which][lax.rem(z + n_kv - j, n_kv)]
        return block.reshape(block.shape[0] * block.shape[1], block.shape[2])

    def token_part(j):
        start = pl.multiple_of(lax.rem(z + n_kv - j, n_kv) * depth, depth)
        return tokens[:, pl.ds(start, depth)]

    def ask(j):
        return remote(
            wanted, asks.at[z], ask_send.at[j], ask_recv.at[j], "kv", lax.rem(z + n_kv - j, n_kv)
        )

    def ask_in(j):
        slot = asks.at[lax.rem(z + j, n_kv)]
        return remote(
            slot, slot, ask_send.at[j], ask_recv.at[j], "kv", lax.rem(z + n_kv - j, n_kv)
        )

    loads[4].wait()
    for j in range(1, n_kv):
        ask(j).start()
    for which in (0, 1):
        for load in (pair_loads, loads[:1])[which]:
            load.wait()
        for j in range(1, n_kv):
            first(which, j).start()
    for j in range(1, n_kv):
        pass_on(0, j)
    for j in range(1, n_kv):
        pass_on(1, j)
        if j == 1:
            for k in range(1, n_kv):
                relay(0, k)
        elif j < n_kv - 1:
            relay(1, j - 1)
    for load in loads[1:4] + loads[5:]:
        load.wait()

    def pair_part(j):
        block = pair_own[...] if j == 0 else pair_all[lax.rem(z + n_kv - j, n_kv)]
        block = jnp.concatenate([block[k] for k in range(n_dp)], axis=1)
        return lax.dot_general(
            token_part(j), block, (((1,), (1,)), ((), ())), preferred_element_type=jnp.float32
        )

    total = pair_part(0)
    for j in range(1, n_kv):
        take(0, j)
        total += pair_part(j)
    kv_own[...] = total.astype(jnp.bfloat16).reshape(blocks, BLOCK_LENGTH, LANES)

    def named(rows_of, owner):
        local = rows_of - owner * blocks
        inside = (local >= 0) & (local < blocks)
        return (
            jnp.min(jnp.where(inside, local, blocks - 1)),
            jnp.max(jnp.where(inside, local, 0)),
        )

    def kv_out(j):
        return remote(
            packed.at[j], kv_far.at[pl.ds(z * CAP, CAP)], kv_send.at[j], kv_recv.at[j],
            "kv", lax.rem(z + j, n_kv),
        )

    def kv_in(j):
        slot = kv_far.at[pl.ds(lax.rem(z + n_kv - j, n_kv) * CAP, CAP)]
        return remote(slot, slot, kv_send.at[j], kv_recv.at[j], "kv", lax.rem(z + j, n_kv))

    kv_far[pl.ds(z * CAP, CAP)] = jnp.zeros((CAP, BLOCK_LENGTH, LANES), jnp.bfloat16)
    for j in range(1, n_kv):
        ask_in(j).wait_recv()
        lowest, highest = named(asks[lax.rem(z + j, n_kv)], z)
        packed[j, 0] = kv_own[lowest]
        packed[j, 1] = kv_own[highest]
    firsts = [named(wanted[...], owner)[0] + owner * blocks for owner in range(n_kv)]
    for j in range(1, n_kv):
        kv_out(j).start()
    for j in range(max(n_kv - 2, 1), n_kv):
        relay(1, j)
    for j in range(1, n_kv):
        first(2, j).start()

    query_sum[...] = jnp.dot(token_part(0), whole(1, 0), preferred_element_type=jnp.float32)
    for j in range(1, n_kv):
        take(1, j)
        query_sum[...] += jnp.dot(token_part(j), whole(1, j), preferred_element_type=jnp.float32)
    query_rows[...] = query_sum[...].astype(jnp.bfloat16) * jnp.bfloat16(HEAD_WIDTH ** (-0.5))

    for j in range(1, n_kv):
        kv_in(j).wait_recv()

    swap = (
        lax.rem(lax.broadcasted_iota(jnp.int32, (LANES, LANES), 0) + HEAD_WIDTH, LANES)
        == lax.broadcasted_iota(jnp.int32, (LANES, LANES), 1)
    ).astype(jnp.float32).astype(jnp.bfloat16)
    for source, start in ((kv_far, 0), (kv_own, n_kv * CAP)):
        count = source.shape[0]
        part = source[...]
        turned = jnp.dot(
            part.reshape(count * BLOCK_LENGTH, LANES), swap, preferred_element_type=jnp.float32
        )
        kv_all[start : start + count] = part
        vk_all[start : start + count] = turned.astype(jnp.bfloat16).reshape(part.shape)

    picks = chosen.shape[1]
    pairs = query_rows.shape[1] // LANES

    def attend(b, carry):
        for j in range(1, n_kv):

            @pl.when(b == min(j, blocks - 1))
            def _(j=j):
                pass_on(2, j)

            @pl.when(b == min(j + 4, blocks - 1))
            def _(j=j):
                relay(2, j)

        lane = lax.broadcasted_iota(jnp.int32, (BLOCK_LENGTH, LANES), 1)
        row = lax.broadcasted_iota(jnp.int32, (BLOCK_LENGTH, LANES), 0)
        low = (lane < HEAD_WIDTH).astype(jnp.float32)
        names = [chosen[b, s] for s in range(picks)]
        offs = [jnp.where(name >= 0, 0.0, HIDDEN) for name in names]
        bias = []
        for s in range(0, picks, 2):
            tile = jnp.where(lane < HEAD_WIDTH, offs[s], offs[s + 1])
            if s == 0:
                tile = jnp.where((lane < HEAD_WIDTH) & (lane > row), HIDDEN, tile)
            bias.append(tile)
        bias = jnp.concatenate(bias, axis=1)

        def place(name):
            name = jnp.maximum(name, 0)
            spot = name - z * blocks + n_kv * CAP
            for owner in range(n_kv):
                local = name - owner * blocks
                away = (local >= 0) & (local < blocks) & (z != owner)
                far = owner * CAP + jnp.where(name == firsts[owner], 0, 1)
                spot = jnp.where(away, far, spot)
            return spot

        safe = [jnp.where(name >= 0, place(name), 0) for name in names]
        kv = jnp.concatenate([kv_all[g] for g in safe], axis=0)
        vk = jnp.concatenate([vk_all[g] for g in safe], axis=0)
        at = pl.ds(pl.multiple_of(b * BLOCK_LENGTH, BLOCK_LENGTH), BLOCK_LENGTH)
        query = query_rows[at, :]
        stacked = jnp.concatenate(
            [query[:, p * LANES : (p + 1) * LANES] for p in range(pairs)], axis=0
        )
        keep = jnp.concatenate([low] * pairs, axis=0)
        outs = []
        for side in range(2):
            mask = keep if side == 0 else 1.0 - keep
            masked = stacked * mask.astype(jnp.bfloat16)
            keys, values = (kv, vk) if side == 0 else (vk, kv)
            scores = lax.dot_general(
                masked, keys, (((1,), (1,)), ((), ())), preferred_element_type=jnp.float32
            )
            scores = scores.reshape(pairs, BLOCK_LENGTH, picks * BLOCK_LENGTH) + bias[None]
            top = jnp.max(scores, axis=2, keepdims=True)
            expon = jnp.exp(scores - top)
            inverse = 1.0 / jnp.sum(expon, axis=2, keepdims=True)
            probs = expon.astype(jnp.bfloat16)
            probs = probs.reshape(pairs * BLOCK_LENGTH, picks * BLOCK_LENGTH)
            out = jnp.dot(probs, values, preferred_element_type=jnp.float32)
            outs.append(out * inverse.reshape(pairs * BLOCK_LENGTH, 1))
        joined = jnp.where(keep > 0.5, outs[0], outs[1]).astype(jnp.bfloat16)
        for p in range(pairs):
            attended[at, p * LANES : (p + 1) * LANES] = joined[
                p * BLOCK_LENGTH : (p + 1) * BLOCK_LENGTH
            ]
        return carry

    lax.fori_loop(0, blocks, attend, 0)

    peer = lax.rem(t + 1, n_tp)
    other_rows = attended[pl.ds(pl.multiple_of(peer * half, half), half), :]
    own_rows = attended[pl.ds(pl.multiple_of(t * half, half), half), :]

    def swap_half(j):
        slot = lax.rem(z + n_kv - j, n_kv)
        return remote(
            leaving.at[slot], arriving.at[slot], t_send.at[j], t_recv.at[j], "tp", peer
        )

    for j in range(n_kv):
        take(2, j)
        weight = whole(2, j)
        slot = lax.rem(z + n_kv - j, n_kv)
        leaving[slot] = jnp.dot(
            other_rows, weight, preferred_element_type=jnp.float32
        ).astype(jnp.bfloat16)
        swap_half(j).start()
        kept[slot] = jnp.dot(own_rows, weight, preferred_element_type=jnp.float32)

    square = jnp.zeros((half, 1), jnp.float32)
    for j in range(n_kv):
        slot = lax.rem(z + n_kv - j, n_kv)
        swap_half(j).wait_recv()
        mixed = kept[slot] + arriving[slot].astype(jnp.float32)
        kept[slot] = mixed
        square += jnp.sum(mixed * mixed, axis=1, keepdims=True)
    scale = lax.rsqrt(square * (1.0 / width) + 1e-06)
    for j in range(n_kv):
        columns = slice(j * depth, (j + 1) * depth)
        result[:, columns] = (kept[j] * scale * gain[:, columns]).astype(jnp.bfloat16)

    for which in range(3):
        for j in range(1, n_kv):
            first(which, j).wait_send()
            for k in (1, 2):
                second(which, j, k).wait_send()
                halfway(which, j, k, near[k]).wait_send()
    for j in range(1, n_kv):
        kv_out(j).wait_send()
        ask(j).wait_send()
    for j in range(n_kv):
        swap_half(j).wait_send()


def per_device_fused(
    n_dp, n_kv, n_tp,
    tokens, chosen, query_weight, key_matrix, value_matrix, out_weight, out_gain,
):
    rows, width = tokens.shape
    depth, columns = query_weight.shape
    blocks = rows // BLOCK_LENGTH
    cut = lambda w: w.reshape(n_dp, w.shape[0] // n_dp, w.shape[1])
    query, out = cut(query_weight), cut(out_weight)
    pair = jax.ShapeDtypeStruct((n_dp, LANES, depth // n_dp), jnp.bfloat16)
    bf16, f32 = jnp.bfloat16, jnp.float32
    vmem = pl.BlockSpec(memory_space=pltpu.VMEM)
    off_core = pl.BlockSpec(memory_space=pltpu.HBM)
    dma = pltpu.SemaphoreType.DMA
    return pl.pallas_call(
        functools.partial(fused, n_dp, n_kv, n_tp),
        out_shape=jax.ShapeDtypeStruct((rows // n_tp, width), bf16),
        in_specs=[
            off_core, off_core, off_core, off_core, off_core, off_core, off_core,
        ],
        out_specs=vmem,
        scratch_shapes=[
            pltpu.SMEM((blocks, chosen.shape[1]), jnp.int32),
            pltpu.VMEM((1, width), f32),
            pltpu.VMEM((rows, width), bf16),
            pltpu.VMEM(pair.shape, bf16),
            pltpu.VMEM(query.shape, bf16),
            pltpu.VMEM(out.shape, bf16),
            pltpu.VMEM((blocks, chosen.shape[1]), jnp.int32),
            pltpu.VMEM((n_kv, blocks, chosen.shape[1]), jnp.int32),
            pltpu.VMEM((n_kv, CAP, BLOCK_LENGTH, LANES), bf16),
            pltpu.VMEM((blocks, BLOCK_LENGTH, LANES), bf16),
            pltpu.VMEM((n_kv * CAP, BLOCK_LENGTH, LANES), bf16),
            pltpu.VMEM((n_kv,) + pair.shape, bf16),
            pltpu.VMEM((n_kv,) + query.shape, bf16),
            pltpu.VMEM((n_kv,) + out.shape, bf16),
            pltpu.VMEM((n_kv * CAP + blocks, BLOCK_LENGTH, LANES), bf16),
            pltpu.VMEM((n_kv * CAP + blocks, BLOCK_LENGTH, LANES), bf16),
            pltpu.VMEM((rows, columns), f32),
            pltpu.VMEM((rows, columns), bf16),
            pltpu.VMEM((rows, columns), bf16),
            pltpu.VMEM((n_kv, rows // n_tp, width // n_kv), bf16),
            pltpu.VMEM((n_kv, rows // n_tp, width // n_kv), bf16),
            pltpu.VMEM((n_kv, rows // n_tp, width // n_kv), f32),
            dma((6 + 2 * n_dp,)), dma((3, n_kv)), dma((3, n_kv)), dma((3, n_kv, 3)), dma((3, n_kv, 3)),
            dma((3, n_kv, 3)), dma((3, n_kv, 3)),
            dma((n_kv,)), dma((n_kv,)), dma((n_kv,)), dma((n_kv,)),
            dma((n_kv,)), dma((n_kv,)),
        ],
        compiler_params=pltpu.CompilerParams(
            collective_id=0, has_side_effects=True, vmem_limit_bytes=54 * 1024 * 1024
        ),
    )(chosen, tokens, key_matrix.T, value_matrix.T, query, out, out_gain.reshape(1, width))


def per_device(tokens, chosen, query_weight, key_matrix, value_matrix, out_weight, out_gain):
    tok_rows = tokens.shape[0]
    blocks = tok_rows // BLOCK_LENGTH
    device = lax.axis_index("kv")
    kv_count = lax.axis_size("kv")
    whole_query, whole_key, whole_value = (
        lax.all_gather(query_weight, "kv", axis=0, tiled=True),
        lax.all_gather(key_matrix, "kv", axis=0, tiled=True),
        lax.all_gather(value_matrix, "kv", axis=0, tiled=True),
    )
    query_rows = jnp.dot(tokens, whole_query, preferred_element_type=jnp.float32).astype(
        jnp.bfloat16
    )
    key_rows = jnp.dot(tokens, whole_key, preferred_element_type=jnp.float32).astype(jnp.bfloat16)
    value_rows = jnp.dot(tokens, whole_value, preferred_element_type=jnp.float32).astype(
        jnp.bfloat16
    )
    paired = jnp.concatenate([key_rows, value_rows], axis=1)
    pair_width = paired.shape[1]
    safe_ids = jnp.maximum(chosen, 0)
    everyone = lax.all_gather(paired, "kv", axis=0, tiled=True).reshape(
        kv_count * blocks, BLOCK_LENGTH, pair_width
    )
    picked = jnp.take(everyone, safe_ids, axis=0)
    head_count = query_rows.shape[1] // HEAD_WIDTH
    grouped = query_rows.reshape(blocks, BLOCK_LENGTH, head_count, HEAD_WIDTH)
    offsets = jnp.arange(BLOCK_LENGTH, dtype=jnp.int32)
    query_pos = (device * blocks + jnp.arange(blocks, dtype=jnp.int32))[
        :, None
    ] * BLOCK_LENGTH + offsets[None, :]
    key_pos = safe_ids[:, :, None] * BLOCK_LENGTH + offsets[None, None, :]
    visible = (chosen >= 0)[:, None, :, None] & (
        key_pos[:, None, :, :] <= query_pos[:, :, None, None]
    )

    def attend_block(inputs):
        query_block, pair_block, seen = inputs
        block_keys = pair_block[..., :HEAD_WIDTH]
        block_values = pair_block[..., HEAD_WIDTH:]
        scores = jnp.einsum(
            "qgd,skd->gqsk", query_block, block_keys, preferred_element_type=jnp.float32
        ) * HEAD_WIDTH ** (-0.5)
        scores = jnp.where(seen[None], scores, -1e30)
        row_max = jnp.max(scores, axis=(2, 3), keepdims=True)
        expon = jnp.exp(scores - row_max)
        row_sum = jnp.sum(expon, axis=(2, 3), keepdims=True)
        weights_bf = (expon / row_sum).astype(jnp.bfloat16)
        result = jnp.einsum(
            "gqsk,skd->qgd", weights_bf, block_values, preferred_element_type=jnp.float32
        )
        return result.astype(jnp.bfloat16)

    attended = lax.map(attend_block, (grouped, picked, visible))
    attended = attended.reshape(tok_rows, head_count * HEAD_WIDTH)
    whole_out = lax.all_gather(out_weight, "kv", axis=1, tiled=True)
    mixed = lax.psum_scatter(
        jnp.dot(attended, whole_out, preferred_element_type=jnp.float32).astype(jnp.bfloat16),
        "tp",
        scatter_dimension=0,
        tiled=True,
    ).astype(jnp.float32)
    normed = mixed * lax.rsqrt(jnp.mean(mixed * mixed, axis=-1, keepdims=True) + 1e-06) * out_gain
    return normed.astype(jnp.bfloat16)


def solution(mesh):
    placed = (
        P(("dp", "kv"), None),
        P(("dp", "kv"), None),
        P("kv", "tp"),
        P("kv", "tp"),
        P("kv", "tp"),
        P("tp", "kv"),
        P(),
    )
    n_dp, n_kv, n_tp = (mesh.shape[name] for name in ("dp", "kv", "tp"))

    def body(tokens, chosen, query_weight, key_matrix, value_matrix, out_weight, out_gain):
        args = (tokens, chosen, query_weight, key_matrix, value_matrix, out_weight, out_gain)
        depth, columns = query_weight.shape
        whole_tiles = (
            depth % (LANES * n_dp) == 0
            and out_weight.shape[0] % (16 * n_dp) == 0
            and out_weight.shape[1] % LANES == 0
            and columns % LANES == 0
            and key_matrix.shape[1] == HEAD_WIDTH
            and chosen.shape[1] % 2 == 0
            and n_tp == 2
            and n_dp == 4
        )
        if whole_tiles:
            return per_device_fused(n_dp, n_kv, n_tp, *args)
        return per_device(*args)

    return jax.shard_map(
        body,
        mesh=mesh,
        in_specs=placed,
        out_specs=P(("dp", "kv", "tp"), None),
        check_vma=False,
    )
```
